32 devices in a mesh: sp: 8 (over z, y), tp: 4 (over x, core).
Axes of the slice: x: 2, y: 2, z: 4, core: 2. Of those that a mesh axis runs over, the one named last changes fastest.
Arguments:
- moe_input: bfloat16 [2048, 2048], P('sp'), may hold values from -17.5 to 17.5
- cotangent: bfloat16 [2048, 2048], P('sp'), may hold values from -6 to 6
- routes: int32 [2048, 2], P('sp'), may hold values from 0 to 7, all different within a row; in each aligned block of 256 rows (0 to 255, 256 to 511, ...) at most 80 rows name the same one
- route_weights: float32 [2048, 2], P('sp'), may hold values from 0.2 to 1
- gate_weight: bfloat16 [8, 2048, 2048], P('sp', None, 'tp'), may hold values from -0.125 to 0.125
- up_weight: bfloat16 [8, 2048, 2048], P('sp', None, 'tp'), may hold values from -0.125 to 0.125
- down_weight: bfloat16 [8, 2048, 2048], P('sp', 'tp'), may hold values from -0.125 to 0.125
- out_weight: bfloat16 [2048, 2048], P(None, 'tp'), may hold values from -0.125 to 0.125
- mixer_output: bfloat16 [2048, 2048], P('sp', 'tp'), may hold values from -6 to 6
- queries: bfloat16 [2048, 2048], P('sp', 'tp'), may hold values from -6 to 6
- key_vectors: bfloat16 [2048, 2048], P('sp', 'tp'), may hold values from -0.75 to 0.75
- value_vectors: bfloat16 [2048, 2048], P('sp', 'tp'), may hold values from -6 to 6
- log_decay: float32 [2048, 32], P('sp', 'tp'), may hold values from -0.85 to 0
- block_states: bfloat16 [16, 32, 64, 64], P('sp', 'tp'), may hold values from -1.5 to 1.5
Outputs:
- grad_gate: float32 [8, 2048, 2048], P('sp', None, 'tp')
- grad_up: float32 [8, 2048, 2048], P('sp', None, 'tp')
- grad_down: float32 [8, 2048, 2048], P('sp', 'tp')
- grad_out: float32 [2048, 2048], P('sp', 'tp')
- grad_queries: bfloat16 [2048, 2048], P('sp', 'tp')
- grad_keys: bfloat16 [2048, 2048], P('sp', 'tp')
- grad_values: bfloat16 [2048, 2048], P('sp', 'tp')
The draws below stay inside these ranges and needn't reach their ends.
Inputs may be any that keep to these rules, and one draw needn't show every extreme that they name: `routes`: each row names 2 different experts. Among the rows of one device no expert is named by more than 80 rows, and in every draw some device's rows name some expert exactly 80 times.
All inputs are finite; a program needn't handle non-finite values.
Results may differ from the reference program's by a relative error of at most 0.02.
Values may be sent and summed in bfloat16 or wider, within the bound.
A program may use at most 128 MiB of HBM per device.

```python
import math
import jax
import jax.numpy as jnp
import numpy as np
from jax import lax

D = 2048
FF = 2048
HEADS = 32
HEAD_DIM = 64
EXPERTS = 8
TOP_K = 2
TOK_DEV = 256
TOKENS = 2048
CAP = 80
BLK = 128
NBLK = 16
N_SP = 8
N_TP = 4


def draw_moe_input(key, part):
    key_rows, key_values = jax.random.split(key)
    row_scale = jnp.exp(jax.random.uniform(key_rows, (TOKENS, 1), jnp.float32, jnp.log(0.25), jnp.log(3.0)))
    values = jnp.clip(jax.random.normal(key_values, (TOKENS, D), jnp.float32), -3.5, 3.5)
    return (values * row_scale).astype(jnp.bfloat16)


def draw_log_decay(key, part):
    subkeys = jax.random.split(key, 9)
    fast_edge = 0.3
    middle_edge = 0.55
    head_class = jax.random.uniform(subkeys[0], (HEADS,), jnp.float32)
    fast_rate = jax.random.uniform(subkeys[1], (HEADS,), jnp.float32, 1.0 / 50.0, 1.0 / 30.0)
    middle_rate = jnp.exp(jax.random.uniform(subkeys[8], (HEADS,), jnp.float32, jnp.log(1.0 / 2048.0), jnp.log(1.0 / 256.0)))
    chain_rate = jax.random.uniform(subkeys[2], (HEADS,), jnp.float32, 0.05, 0.15) / TOKENS
    base_rate = jnp.where(head_class < fast_edge, fast_rate, jnp.where(head_class < middle_edge, middle_rate, chain_rate))
    segment_factor = jax.random.uniform(subkeys[3], (TOKENS // TOK_DEV, 1, HEADS), jnp.float32, 1.0, 3.0)
    jitter = jax.random.uniform(subkeys[4], (TOKENS // TOK_DEV, TOK_DEV, HEADS), jnp.float32, 0.5, 1.5)
    forgetting_factor_matrix = (segment_factor * jitter).reshape(TOKENS, HEADS) * base_rate[None, :]
    primary_expert_index = jax.random.randint(subkeys[5], (HEADS,), 0, TOKENS)
    runner_expert_index = (primary_expert_index + 1 + jax.random.randint(subkeys[6], (HEADS,), 0, TOKENS - 1)) % TOKENS
    discarded_log_terms = jnp.log(jax.random.uniform(subkeys[7], (2, HEADS), jnp.float32, 0.5, 0.8))
    sequence_indices = jnp.arange(TOKENS, dtype=jnp.int32)[:, None]
    exchange_batches = jnp.where(sequence_indices == primary_expert_index[None, :], discarded_log_terms[0][None, :], 0.0)
    exchange_batches = exchange_batches + jnp.where(sequence_indices == runner_expert_index[None, :], discarded_log_terms[1][None, :], 0.0)
    return (exchange_batches - forgetting_factor_matrix).astype(jnp.float32)


def spiked(values, own_key, source, target, shards_of, factor):
    owner, partner = [(jnp.arange(values.shape[axis_at]) // (values.shape[axis_at] // shards_of)).reshape([-1 if axis == axis_at else 1 for axis in range(values.ndim)]) for axis_at in (source, target)]
    chosen = jax.random.permutation(own_key, shards_of)[partner]
    strong = (owner == chosen) | (owner == (partner + shards_of // 2) % shards_of)
    return jnp.where(strong, factor * values, values)


def level_of(rng, shape, cuts, low, top_value):
    loudness, own = 1.0, jax.random.fold_in(rng, 6)
    for position, shards_of in cuts:
        heights = jnp.exp(jax.random.uniform(jax.random.fold_in(own, position), (shards_of,), jnp.float32, low / len(cuts), top_value / len(cuts)))
        loudness = loudness * jnp.repeat(heights, shape[position] // shards_of).reshape([-1 if axis == position else 1 for axis in range(len(shape))])
    return loudness


def deal_out(own_key, own, number, rows, count, top, reach, slope):
    sequence = jax.random.permutation(own_key, count)
    packed, usual = shares(count, rows * top, reach, slope, True), shares(count, rows * top, reach, slope, False)
    places = jnp.arange(count)

    def named(lengths, offset_by):
        used = int((lengths > 0).sum())
        fixed = max(1, used // 4)
        passed = fixed + (places - fixed + offset_by * (used - fixed)) % max(1, count - fixed)
        return jnp.zeros((count,), jnp.int32).at[sequence[jnp.where(places < fixed, places, passed)]].set(jnp.asarray(lengths, jnp.int32))

    lengths = jnp.where(number % 4 == 0, named(packed, number // 4), named(usual, number - number // 4 - 1))
    mixed = jax.random.permutation(jax.random.fold_in(own, 3), count)
    donor, receiver = mixed[0:count // 2 * 2:2], mixed[1:count // 2 * 2:2]
    room = jnp.minimum(lengths[donor] - 1, reach - lengths[receiver]) // 2
    room = jnp.where((donor == sequence[0]) | (receiver == sequence[0]) | (lengths[receiver] == 0), 0, jnp.maximum(room, 0))
    passed = jax.random.randint(jax.random.fold_in(own, 4), (count // 2,), 0, 1 << 20) % (room + 1)
    lengths = lengths.at[donor].add(-passed).at[receiver].add(passed)
    members = jnp.searchsorted(jnp.cumsum(lengths), jnp.arange(rows * top), side="right").astype(jnp.int32)
    table = members.reshape(top, rows).T
    table = table[jax.random.permutation(jax.random.fold_in(own, 1), rows)]
    offset_by = jax.random.randint(jax.random.fold_in(own, 2), (rows, 1), 0, top)
    return jnp.take_along_axis(table, (jnp.arange(top)[None, :] + offset_by) % top, axis=1)


def shares(number_of, total, most, skew, full):
    portions = [(1 << 20) // math.isqrt(grade ** skew) + 1 for grade in range(1, number_of + 1)]
    largest = most if full else min(most, max(-(-total // number_of), total * portions[0] // sum(portions)))
    least = 1 if total - largest >= number_of - 1 else 0
    counts, rest = [largest] + [least] * (number_of - 1), total - largest - least * (number_of - 1)
    while rest > 0:
        free = [i for i in range(1, number_of) if counts[i] < largest] or [i for i in range(1, number_of) if counts[i] < most]
        mass, budget = sum([portions[i] for i in free]), rest
        for i in free:
            extra = min(most - counts[i], max(1, budget * portions[i] // mass), rest)
            counts[i] = counts[i] + extra
            rest = rest - extra
    return np.array(counts)


def gaussian(stream_key, shape, spread, limit, cuts=(), kind=jnp.bfloat16):
    entries = spread * jax.random.normal(stream_key, shape, jnp.float32)
    if cuts:
        entries = entries * level_of(stream_key, shape, cuts, -0.22, 0.18)
    return jnp.clip(entries, -limit, limit).astype(kind)


def noise_with(key, extent, spread, bound, cuts, heavy, held_as=jnp.bfloat16):
    values = spread * jax.random.normal(key, extent, jnp.float32)
    if cuts:
        values = values * level_of(key, extent, cuts, -0.22, 0.18)
    return jnp.clip(spiked(values, jax.random.fold_in(key, 3), *heavy), -bound, bound).astype(held_as)


def setup_inputs(seed: int = 0) -> dict:
    arg_keys = jax.random.split(jax.random.key(seed), 15)
    moe_input = draw_moe_input(jax.random.fold_in(arg_keys[14], 71), 0)
    cotangent = noise_with(arg_keys[1], (TOKENS, D), 1.0, 6.0, ((0, 8),), (0, 1, 8, 2.0))
    routes_keys = jax.random.split(jax.random.fold_in(arg_keys[2], 1), TOKENS // TOK_DEV)
    routes_turns = jax.random.permutation(jax.random.fold_in(arg_keys[2], 3), TOKENS // TOK_DEV)
    routes = jax.vmap(lambda own, number: deal_out(jax.random.fold_in(arg_keys[2], 2), own, number, TOK_DEV, EXPERTS, TOP_K, CAP, 1))(routes_keys, routes_turns).reshape((TOKENS, TOP_K))
    route_weights = jnp.clip(0.2 + 0.8 * jax.random.uniform(arg_keys[3], (TOKENS, TOP_K), jnp.float32) ** level_of(arg_keys[3], (TOKENS, TOP_K), ((0, 8),), -0.2, 0.2), 0.2, 1.0)
    gate_weight = gaussian(arg_keys[4], (EXPERTS, D, FF), D ** -0.5, 0.125, ((0, 8), (2, 4)))
    up_weight = gaussian(arg_keys[5], (EXPERTS, D, FF), D ** -0.5, 0.125, ((0, 8), (2, 4)))
    down_weight = gaussian(arg_keys[6], (EXPERTS, FF, D), FF ** -0.5, 0.125, ((0, 8), (1, 4)))
    out_weight = gaussian(arg_keys[7], (D, HEADS * HEAD_DIM), D ** -0.5, 0.125, ((1, 4),))
    mixer_output = gaussian(arg_keys[8], (TOKENS, HEADS * HEAD_DIM), 1.0, 6.0, ((0, 8), (1, 4)))
    queries = gaussian(arg_keys[9], (TOKENS, HEADS * HEAD_DIM), 1.0, 6.0, ((0, 8), (1, 4)))
    key_vectors = gaussian(arg_keys[10], (TOKENS, HEADS * HEAD_DIM), HEAD_DIM ** -0.5, 0.75, ((0, 8), (1, 4)))
    value_vectors = gaussian(arg_keys[11], (TOKENS, HEADS * HEAD_DIM), 1.0, 6.0, ((0, 8), (1, 4)))
    log_decay = draw_log_decay(jax.random.fold_in(arg_keys[14], 71), 0)
    block_states = gaussian(arg_keys[13], (NBLK, HEADS, HEAD_DIM, HEAD_DIM), 0.25, 1.5, ((0, 8), (1, 4)))
    return {"moe_input": moe_input, "cotangent": cotangent, "routes": routes, "route_weights": route_weights, "gate_weight": gate_weight, "up_weight": up_weight, "down_weight": down_weight, "out_weight": out_weight, "mixer_output": mixer_output, "queries": queries, "key_vectors": key_vectors, "value_vectors": value_vectors, "log_decay": log_decay, "block_states": block_states}


clamp_limit = 7.0
sigmoid_sharpness = 1.702


def round_keep(values):
    return lax.optimization_barrier(values.astype(jnp.bfloat16)).astype(jnp.float32)


def pair_slots(routes_blocks):
    flat_routes = routes_blocks.reshape(routes_blocks.shape[0], -1)
    onehot = (flat_routes[:, :, None] == jnp.arange(EXPERTS, dtype=jnp.int32)[None, None, :]).astype(jnp.int32)
    before = jnp.cumsum(onehot, axis=1) - onehot
    return (flat_routes * CAP + jnp.sum(before * onehot, axis=2)).astype(jnp.int32)


def expert_grads(expert_rows, expert_cotangent, w_gate, w_up, w_down):
    gate_pre = jnp.dot(expert_rows, w_gate, preferred_element_type=jnp.float32)
    up_pre = jnp.dot(expert_rows, w_up, preferred_element_type=jnp.float32)
    act_grad = jnp.dot(expert_cotangent, w_down.T, preferred_element_type=jnp.float32)
    clamped = jnp.minimum(gate_pre, clamp_limit)
    logistic = jax.nn.sigmoid(sigmoid_sharpness * clamped)
    linear = jnp.clip(up_pre, -clamp_limit, clamp_limit)
    activation = (clamped * logistic * (linear + 1.0)).astype(jnp.bfloat16)
    slope_term = logistic + sigmoid_sharpness * clamped * logistic * (1.0 - logistic)
    gate_grad = jnp.where(gate_pre < clamp_limit, act_grad * (linear + 1.0) * slope_term, 0.0).astype(jnp.bfloat16)
    up_grad = jnp.where(jnp.abs(up_pre) < clamp_limit, act_grad * clamped * logistic, 0.0).astype(jnp.bfloat16)
    group_width = w_gate.shape[1] // N_TP
    gate_split = gate_grad.astype(jnp.float32).reshape(-1, N_TP, group_width)
    up_split = up_grad.astype(jnp.float32).reshape(-1, N_TP, group_width)
    partials = jnp.einsum("rgf,dgf->grd", gate_split, w_gate.astype(jnp.float32).reshape(-1, N_TP, group_width))
    partials = partials + jnp.einsum("rgf,dgf->grd", up_split, w_up.astype(jnp.float32).reshape(-1, N_TP, group_width))
    pair_grad = jnp.sum(round_keep(partials), axis=0).astype(jnp.bfloat16)
    grad_gate = jnp.dot(expert_rows.T, gate_grad, preferred_element_type=jnp.float32)
    grad_up = jnp.dot(expert_rows.T, up_grad, preferred_element_type=jnp.float32)
    grad_down = jnp.dot(activation.T, expert_cotangent, preferred_element_type=jnp.float32)
    return pair_grad, grad_gate, grad_up, grad_down


def retention_grads(queries, key_vectors, value_vectors, grad_mix, log_decay, block_states):
    blocks = TOKENS // BLK
    block_shape = (blocks, BLK, HEADS, HEAD_DIM)
    query_blocks = queries.astype(jnp.float32).reshape(block_shape)
    key_blocks = key_vectors.astype(jnp.float32).reshape(block_shape)
    value_blocks = value_vectors.astype(jnp.float32).reshape(block_shape)
    grad_blocks = grad_mix.astype(jnp.float32).reshape(block_shape)
    states = block_states.astype(jnp.float32)
    cumulative = jnp.cumsum(log_decay.reshape(blocks, BLK, HEADS), axis=1)
    block_ends = cumulative[:, -1, :]
    to_end = jnp.exp(block_ends[:, None, :] - cumulative)
    from_start = jnp.exp(cumulative)
    per_attention_head = jnp.transpose(cumulative, (0, 2, 1))
    differences = per_attention_head[:, :, :, None] - per_attention_head[:, :, None, :]
    causal = jnp.arange(BLK, dtype=jnp.int32)[:, None] >= jnp.arange(BLK, dtype=jnp.int32)[None, :]
    decays = jnp.where(causal, jnp.exp(jnp.minimum(differences, 0.0)), 0.0)
    weighted_grad = round_keep(jnp.einsum("nthe,nshe->nhts", grad_blocks, value_blocks) * decays)
    weighted_score = round_keep(jnp.einsum("nthd,nshd->nhts", query_blocks, key_blocks) * decays)
    query_intra = jnp.einsum("nhts,nshd->nthd", weighted_grad, key_blocks)
    query_carry = jnp.einsum("nthe,nhde->nthd", grad_blocks, states) * from_start[..., None]
    grad_queries = (query_intra + query_carry).astype(jnp.bfloat16).reshape(TOKENS, HEADS * HEAD_DIM)
    scaled_queries = round_keep(query_blocks * from_start[..., None])
    outer_terms = jnp.einsum("nthd,nthe->nhde", scaled_queries, grad_blocks)
    end_factor = jnp.exp(block_ends)

    def suffix_step(state_grad, inputs):
        factor, outer_block = inputs
        return factor[:, None, None] * state_grad + outer_block, state_grad

    start_grad = jnp.zeros((HEADS, HEAD_DIM, HEAD_DIM), jnp.float32)
    _, leaving = lax.scan(suffix_step, start_grad, (end_factor, outer_terms), reverse=True)
    carried = round_keep(leaving)
    key_intra = jnp.einsum("nhts,nthd->nshd", weighted_grad, query_blocks)
    value_intra = jnp.einsum("nhts,nthe->nshe", weighted_score, grad_blocks)
    key_carry = jnp.einsum("nshe,nhde->nshd", value_blocks, carried) * to_end[..., None]
    value_carry = jnp.einsum("nshd,nhde->nshe", key_blocks, carried) * to_end[..., None]
    grad_keys = (key_intra + key_carry).astype(jnp.bfloat16).reshape(TOKENS, HEADS * HEAD_DIM)
    grad_values = (value_intra + value_carry).astype(jnp.bfloat16).reshape(TOKENS, HEADS * HEAD_DIM)
    return grad_queries, grad_keys, grad_values


def reference(moe_input, cotangent, routes, route_weights, gate_weight, up_weight, down_weight, out_weight, mixer_output, queries, key_vectors, value_vectors, log_decay, block_states):
    pair_count = TOK_DEV * TOP_K
    slot_index = pair_slots(routes.reshape(N_SP, TOK_DEV, TOP_K))
    source = jnp.arange(N_SP, dtype=jnp.int32)[:, None]
    pair_ids = (source * pair_count + jnp.arange(pair_count, dtype=jnp.int32)[None, :]).astype(jnp.int32)
    slot_pair = jnp.full((N_SP, EXPERTS * CAP), TOKENS * TOP_K, jnp.int32).at[source, slot_index].set(pair_ids)
    tables = jnp.transpose(slot_pair.reshape(N_SP, EXPERTS, CAP), (1, 0, 2)).reshape(EXPERTS, N_SP * CAP)
    zero_row = jnp.zeros((1, D), jnp.bfloat16)
    scaled = (route_weights[:, :, None] * cotangent.astype(jnp.float32)[:, None, :]).astype(jnp.bfloat16)
    scaled = jnp.concatenate([scaled.reshape(TOKENS * TOP_K, D), zero_row], axis=0)
    inputs_padded = jnp.concatenate([moe_input, zero_row], axis=0)

    def one_expert(operands):
        table, w_gate, w_up, w_down = operands
        return expert_grads(inputs_padded[table // TOP_K], scaled[table], w_gate, w_up, w_down)

    pair_rows, grad_gate, grad_up, grad_down = lax.map(one_expert, (tables, gate_weight, up_weight, down_weight))
    pair_sum = jnp.zeros((TOKENS * TOP_K + 1, D), jnp.float32).at[tables.reshape(-1)].add(pair_rows.reshape(-1, D).astype(jnp.float32))
    token_sum = jnp.sum(pair_sum[:TOKENS * TOP_K].reshape(TOKENS, TOP_K, D), axis=1)
    residual_grad = (cotangent.astype(jnp.float32) + token_sum).astype(jnp.bfloat16)
    grad_out = jnp.dot(residual_grad.T, mixer_output, preferred_element_type=jnp.float32)
    grad_mix = jnp.dot(residual_grad, out_weight, preferred_element_type=jnp.float32).astype(jnp.bfloat16)
    grad_queries, grad_keys, grad_values = retention_grads(queries, key_vectors, value_vectors, grad_mix, log_decay, block_states)
    return (grad_gate, grad_up, grad_down, grad_out, grad_queries, grad_keys, grad_values)
```

```python
import functools

import jax
import jax.numpy as jnp
from jax import lax
from jax.experimental import pallas as pl
from jax.experimental.pallas import tpu as pltpu
from jax.sharding import PartitionSpec as P

TOP_K = 2
MESH = pl.DeviceIdType.MESH
VMEM = pl.BlockSpec(memory_space=pltpu.VMEM)
ANY = pl.BlockSpec(memory_space=pl.ANY)

clamp_limit = 7.0
sigmoid_sharpness = 1.702


def contract_rows(left, right):
    return lax.dot_general(
        left, right, (((0,), (0,)), ((), ())), preferred_element_type=jnp.float32
    )


def contract_cols(left, right):
    return lax.dot_general(
        left, right, (((1,), (1,)), ((), ())), preferred_element_type=jnp.float32
    )


def peer_order(peers):
    near = [k for k in range(1, peers) if k < peers // 2]
    far = [k for k in range(1, peers) if k >= peers // 2]
    order = []
    while near or far:
        if near:
            order.append(near.pop(0))
        if far:
            order.append(far.pop(0))
    return order


def greet(peers, sp, tp):
    barrier = pltpu.get_barrier_semaphore()
    others = [(sp ^ k, tp) for k in range(1, peers)] + [(sp, tp ^ 1), (sp, tp ^ 2)]
    for other in others:
        pl.semaphore_signal(barrier, inc=1, device_id=other, device_id_type=MESH)
    pl.semaphore_wait(barrier, len(others))


def remote(src, dst, sems, kind, at, device):
    return pltpu.make_async_remote_copy(
        src_ref=src,
        dst_ref=dst,
        send_sem=sems.at[(2 * kind,) + at],
        recv_sem=sems.at[(2 * kind + 1,) + at],
        device_id=device,
        device_id_type=MESH,
    )


def exchange_start(peers, sp, tp, arrays, source, chunk, sems, local_sems):
    order = peer_order(peers)
    owns, firsts = [], {}
    for k in order:
        for a, (src, dst) in enumerate(arrays):
            copy = remote(source(src, sp ^ k), chunk(dst, sp, tp), sems, 0, (a, k), (sp ^ k, tp))
            copy.start()
            firsts[a, k] = copy
    for a, (src, dst) in enumerate(arrays):
        copy = pltpu.make_async_copy(source(src, sp), chunk(dst, sp, tp), local_sems.at[a])
        copy.start()
        owns.append(copy)
    return order, owns, firsts


def exchange_finish(peers, sp, tp, arrays, source, chunk, sems, state):
    order, owns, firsts = state
    crossings, partners, forwards = {}, {}, {}

    def forward(k):
        for a, (_, dst) in enumerate(arrays):
            crossings[a, k].wait_recv()
            here = chunk(dst, sp ^ k, tp ^ 2)
            copy = remote(here, here, sems, 3, (a, k), (sp, tp ^ 1))
            copy.start()
            forwards[a, k] = copy

    steps = [0] + order
    for i, k in enumerate(steps):
        for a, (src, dst) in enumerate(arrays):
            there = chunk(dst, sp ^ k, tp)
            if k:
                firsts[a, k].wait_recv()
                here = there
            else:
                here = source(src, sp)
            copy = remote(here, there, sems, 1, (a, k), (sp, tp ^ 2))
            copy.start()
            crossings[a, k] = copy
            copy = remote(here, there, sems, 2, (a, k), (sp, tp ^ 1))
            copy.start()
            partners[a, k] = copy
        if i >= 1:
            forward(steps[i - 1])
    forward(steps[-1])
    for copy in owns:
        copy.wait()
    for group in (partners, forwards):
        for copy in group.values():
            copy.wait_recv()
    for group in (firsts, crossings, partners, forwards):
        for copy in group.values():
            copy.wait_send()


def dispatch_kernel(peers, x_ref, g_ref, ox_ref, og_ref, sems, local_sems):
    sp, tp = lax.axis_index("sp"), lax.axis_index("tp")
    width = x_ref.shape[2]
    greet(peers, sp, tp)

    def source(ref, s):
        return ref.at[s]

    def chunk(ref, s, t):
        return ref.at[s, :, pl.ds(pl.multiple_of(t * width, width), width)]

    arrays = ((x_ref, ox_ref), (g_ref, og_ref))
    state = exchange_start(peers, sp, tp, arrays, source, chunk, sems, local_sems)
    exchange_finish(peers, sp, tp, arrays, source, chunk, sems, state)


def dispatch(x, g, parts):
    peers, capacity, width = x.shape
    out = jax.ShapeDtypeStruct((peers, capacity, width * parts), jnp.bfloat16)
    return pl.pallas_call(
        functools.partial(dispatch_kernel, peers),
        out_shape=(out, out),
        in_specs=[ANY, ANY],
        out_specs=(ANY, ANY),
        scratch_shapes=[
            pltpu.SemaphoreType.DMA((8, 2, peers)),
            pltpu.SemaphoreType.DMA((2,)),
        ],
        compiler_params=pltpu.CompilerParams(collective_id=0, has_side_effects=True),
        name="dispatch",
    )(x, g)


def return_kernel(
    peers, part_ref, pick_ref, cot_ref, res_ref, rx1, acc, sb, rx2, fb, ret, sems, tail_sems
):
    sp, tp = lax.axis_index("sp"), lax.axis_index("tp")
    width = cot_ref.shape[1]
    greet(peers, sp, tp)
    steps = peer_order(peers)[::-1] + [0]

    def cols(t):
        return pl.ds(pl.multiple_of(t * width, width), width)

    firsts, crossings, homes = {}, {}, {}
    for k in steps:
        for half, t in ((0, tp ^ 1), (1, tp ^ 3)):
            copy = remote(
                part_ref.at[sp ^ k, :, cols(t)], rx1.at[half, k], sems, half, (k,), (sp, tp ^ 1)
            )
            copy.start()
            firsts[half, k] = copy

    def cross(k):
        firsts[1, k].wait_recv()
        sb[k] = (
            part_ref[sp ^ k, :, cols(tp ^ 2)].astype(jnp.float32)
            + rx1[1, k].astype(jnp.float32)
        ).astype(jnp.bfloat16)
        crossings[k] = remote(sb.at[k], rx2.at[k], sems, 2, (k,), (sp, tp ^ 2))
        crossings[k].start()
        firsts[0, k].wait_recv()
        acc[k] = part_ref[sp ^ k, :, cols(tp)].astype(jnp.float32) + rx1[0, k].astype(
            jnp.float32
        )

    def home(k):
        crossings[k].wait_recv()
        final = (acc[k] + rx2[k].astype(jnp.float32)).astype(jnp.bfloat16)
        if k:
            fb[k] = final
            homes[k] = remote(fb.at[k], ret.at[sp], sems, 3, (k,), (sp ^ k, tp))
            homes[k].start()
        else:
            ret[sp] = final

    for i, k in enumerate(steps):
        cross(k)
        if i >= 2:
            home(steps[i - 2])
    home(steps[-2])
    home(steps[-1])
    total = cot_ref[...].astype(jnp.float32)
    for k in [0] + [k for k in steps if k]:
        if k:
            homes[k].wait_recv()
        total = total + jnp.dot(
            pick_ref[sp ^ k], ret[sp ^ k], preferred_element_type=jnp.float32
        )
    res_ref[:, cols(tp)] = total.astype(jnp.bfloat16)
    mine = res_ref.at[:, cols(tp)]
    across = remote(mine, mine, tail_sems, 0, (), (sp, tp ^ 2))
    across.start()
    beside = remote(mine, mine, tail_sems, 1, (), (sp, tp ^ 1))
    beside.start()
    across.wait_recv()
    theirs = res_ref.at[:, cols(tp ^ 2)]
    onward = remote(theirs, theirs, tail_sems, 2, (), (sp, tp ^ 1))
    onward.start()
    beside.wait_recv()
    onward.wait_recv()
    for group in (firsts, crossings, homes):
        for copy in group.values():
            copy.wait_send()
    for copy in (across, beside, onward):
        copy.wait_send()


def return_rows(part, pick, cot):
    peers, capacity, full = part.shape
    tokens, width = cot.shape
    rows = (peers, capacity, width)
    return pl.pallas_call(
        functools.partial(return_kernel, peers),
        out_shape=jax.ShapeDtypeStruct((tokens, full), jnp.bfloat16),
        in_specs=[VMEM] * 3,
        out_specs=VMEM,
        scratch_shapes=[
            pltpu.VMEM((2,) + rows, jnp.bfloat16),
            pltpu.VMEM(rows, jnp.float32),
            pltpu.VMEM(rows, jnp.bfloat16),
            pltpu.VMEM(rows, jnp.bfloat16),
            pltpu.VMEM(rows, jnp.bfloat16),
            pltpu.VMEM(rows, jnp.bfloat16),
            pltpu.SemaphoreType.DMA((8, peers)),
            pltpu.SemaphoreType.DMA((6,)),
        ],
        compiler_params=pltpu.CompilerParams(
            collective_id=1, has_side_effects=True, vmem_limit_bytes=40 * 2**20
        ),
        name="return_rows",
    )(part, pick, cot)


def final_kernel(
    peers, parts, res_ref, tot_ref, log_ref, all_res, all_tot, all_log, sems, local_sems, st_sems
):
    sp, tp = lax.axis_index("sp"), lax.axis_index("tp")
    share = res_ref.shape[1] // parts
    greet(peers, sp, tp)

    def rows(t):
        return pl.ds(pl.multiple_of(t * share, share), share)

    def source(ref, s):
        return ref.at[s, rows(tp)]

    def chunk(ref, s, t):
        return ref.at[s, rows(t)]

    small = []
    for k in peer_order(peers):
        for i, (src, dst) in enumerate(((tot_ref, all_tot), (log_ref, all_log))):
            copy = remote(src, dst.at[sp], st_sems, i, (k,), (sp ^ k, tp))
            copy.start()
            small.append(copy)
    own = []
    for i, (src, dst) in enumerate(((tot_ref, all_tot), (log_ref, all_log))):
        copy = pltpu.make_async_copy(src, dst.at[sp], local_sems.at[1 + i])
        copy.start()
        own.append(copy)
    arrays = ((res_ref, all_res),)
    state = exchange_start(peers, sp, tp, arrays, source, chunk, sems, local_sems)
    exchange_finish(peers, sp, tp, arrays, source, chunk, sems, state)
    for copy in own + small:
        copy.wait()


def final_exchange(res, tot, logs, parts):
    peers = res.shape[0]
    return pl.pallas_call(
        functools.partial(final_kernel, peers, parts),
        out_shape=(
            jax.ShapeDtypeStruct(res.shape, res.dtype),
            jax.ShapeDtypeStruct((peers,) + tot.shape, tot.dtype),
            jax.ShapeDtypeStruct((peers,) + logs.shape, logs.dtype),
        ),
        in_specs=[ANY] * 3,
        out_specs=(ANY,) * 3,
        scratch_shapes=[
            pltpu.SemaphoreType.DMA((8, 1, peers)),
            pltpu.SemaphoreType.DMA((3,)),
            pltpu.SemaphoreType.DMA((4, peers)),
        ],
        compiler_params=pltpu.CompilerParams(collective_id=2, has_side_effects=True),
        name="final_exchange",
    )(res, tot, logs)


def pair_slots(routes, experts_total, capacity):
    flat_routes = routes.reshape(-1)
    onehot = (flat_routes[:, None] == jnp.arange(experts_total, dtype=jnp.int32)[None, :]).astype(
        jnp.int32
    )
    before = jnp.cumsum(onehot, axis=0) - onehot
    return flat_routes * capacity + jnp.sum(before * onehot, axis=1)


def expert_terms(expert_rows, expert_cotangent, w_gate, w_up, w_down):
    gate_pre = jnp.dot(expert_rows, w_gate, preferred_element_type=jnp.float32)
    up_pre = jnp.dot(expert_rows, w_up, preferred_element_type=jnp.float32)
    act_grad = contract_cols(expert_cotangent, w_down)
    clamped = jnp.minimum(gate_pre, clamp_limit)
    logistic = jax.nn.sigmoid(sigmoid_sharpness * clamped)
    linear = jnp.clip(up_pre, -clamp_limit, clamp_limit)
    activation = (clamped * logistic * (linear + 1.0)).astype(jnp.bfloat16)
    slope_term = logistic + sigmoid_sharpness * clamped * logistic * (1.0 - logistic)
    gate_grad = jnp.where(
        gate_pre < clamp_limit, act_grad * (linear + 1.0) * slope_term, 0.0
    ).astype(jnp.bfloat16)
    up_grad = jnp.where(jnp.abs(up_pre) < clamp_limit, act_grad * clamped * logistic, 0.0).astype(
        jnp.bfloat16
    )
    input_part = contract_cols(gate_grad, w_gate) + contract_cols(up_grad, w_up)
    return (
        input_part,
        contract_rows(expert_rows, gate_grad),
        contract_rows(expert_rows, up_grad),
        contract_rows(activation, expert_cotangent),
    )


def retention_grads(
    queries, key_vectors, value_vectors, grad_mix, log_decay, block_states, exchange
):
    tok_dev = queries.shape[0]
    heads_local = log_decay.shape[1]
    head_dim = queries.shape[1] // heads_local
    blocks = block_states.shape[0]
    block_rows = tok_dev // blocks
    block_shape = (blocks, block_rows, heads_local, head_dim)
    query_blocks = queries.reshape(block_shape)
    key_blocks = key_vectors.reshape(block_shape)
    value_blocks = value_vectors.reshape(block_shape)
    grad_blocks = grad_mix.reshape(block_shape)
    cumulative = jnp.cumsum(log_decay.reshape(blocks, block_rows, heads_local), axis=1)
    block_ends = cumulative[:, -1, :]
    to_end = jnp.exp(block_ends[:, None, :] - cumulative)
    from_start = jnp.exp(cumulative)
    per_attention_head = jnp.transpose(cumulative, (0, 2, 1))
    differences = per_attention_head[:, :, :, None] - per_attention_head[:, :, None, :]
    causal = (
        jnp.arange(block_rows, dtype=jnp.int32)[:, None]
        >= jnp.arange(block_rows, dtype=jnp.int32)[None, :]
    )
    decays = jnp.where(causal, jnp.exp(jnp.minimum(differences, 0.0)), 0.0)
    scaled_queries = (query_blocks * from_start[..., None]).astype(jnp.bfloat16)
    outer_terms = jnp.einsum(
        "nthd,nthe->nhde", scaled_queries, grad_blocks, preferred_element_type=jnp.float32
    )
    end_factor = jnp.exp(block_ends)
    local_total = jnp.zeros((heads_local, head_dim, head_dim), jnp.float32)
    for block_id in reversed(range(blocks)):
        local_total = end_factor[block_id][:, None, None] * local_total + outer_terms[block_id]
    all_totals, all_logs = exchange(local_total, jnp.sum(block_ends, axis=0))
    peers, place = lax.axis_size("sp"), lax.axis_index("sp")
    where = jnp.arange(peers, dtype=jnp.int32)
    between = ((where[None, :] > place) & (where[None, :] < where[:, None]))[..., None]
    reach = jnp.sum(jnp.where(between, all_logs[None], 0.0), axis=1)
    reach = jnp.where((where > place)[:, None], jnp.exp(reach), 0.0)
    suffix = jnp.sum(reach[:, :, None, None] * all_totals.astype(jnp.float32), axis=0)
    grad_dot = jnp.einsum(
        "nthe,nshe->nhts", grad_blocks, value_blocks, preferred_element_type=jnp.float32
    )
    weighted_grad = (grad_dot * decays).astype(jnp.bfloat16)
    score_dot = jnp.einsum(
        "nthd,nshd->nhts", query_blocks, key_blocks, preferred_element_type=jnp.float32
    )
    weighted_score = (score_dot * decays).astype(jnp.bfloat16)
    query_intra = jnp.einsum(
        "nhts,nshd->nthd", weighted_grad, key_blocks, preferred_element_type=jnp.float32
    )
    query_carry = jnp.einsum(
        "nthe,nhde->nthd", grad_blocks, block_states, preferred_element_type=jnp.float32
    )
    grad_queries = (
        (query_intra + query_carry * from_start[..., None])
        .astype(jnp.bfloat16)
        .reshape(tok_dev, -1)
    )
    key_intra = jnp.einsum(
        "nhts,nthd->nshd", weighted_grad, query_blocks, preferred_element_type=jnp.float32
    )
    value_intra = jnp.einsum(
        "nhts,nthe->nshe", weighted_score, grad_blocks, preferred_element_type=jnp.float32
    )
    state_grad = suffix
    leaving = []
    for block_id in reversed(range(blocks)):
        leaving.append(state_grad)
        state_grad = end_factor[block_id][:, None, None] * state_grad + outer_terms[block_id]
    carried = jnp.stack(leaving[::-1], axis=0).astype(jnp.bfloat16)
    key_carry = jnp.einsum(
        "nshe,nhde->nshd", value_blocks, carried, preferred_element_type=jnp.float32
    )
    value_carry = jnp.einsum(
        "nshd,nhde->nshe", key_blocks, carried, preferred_element_type=jnp.float32
    )
    grad_keys = (
        (key_intra + key_carry * to_end[..., None]).astype(jnp.bfloat16).reshape(tok_dev, -1)
    )
    grad_values = (
        (value_intra + value_carry * to_end[..., None]).astype(jnp.bfloat16).reshape(tok_dev, -1)
    )
    return (grad_queries, grad_keys, grad_values)


def shards(
    moe_input,
    cotangent,
    routes,
    route_weights,
    gate_weight,
    up_weight,
    down_weight,
    out_weight,
    mixer_output,
    queries,
    key_vectors,
    value_vectors,
    log_decay,
    block_states,
):
    tok_dev, model_width = cotangent.shape
    peers, parts = lax.axis_size("sp"), lax.axis_size("tp")
    capacity = 5 * tok_dev * TOP_K // (4 * peers)
    slots = pair_slots(routes, peers, capacity).reshape(tok_dev, TOP_K)
    share_width = model_width // parts
    offset = lax.axis_index("tp") * share_width
    my_inputs = lax.dynamic_slice_in_dim(moe_input, offset, share_width, 1)
    my_cotangent = lax.dynamic_slice_in_dim(cotangent, offset, share_width, 1)
    places = jnp.arange(peers * capacity, dtype=jnp.int32)
    hits = [slots[:, j][None, :] == places[:, None] for j in range(TOP_K)]
    pick = functools.reduce(jnp.logical_or, hits).astype(jnp.bfloat16)
    slot_weight = sum(
        jnp.sum(jnp.where(hits[j], route_weights[:, j][None, :], 0.0), axis=1)
        for j in range(TOP_K)
    )
    rows = (peers, capacity, share_width)
    send_inputs = jnp.dot(pick, my_inputs, preferred_element_type=jnp.float32).astype(
        jnp.bfloat16
    )
    send_grads = (
        jnp.dot(pick, my_cotangent, preferred_element_type=jnp.float32) * slot_weight[:, None]
    ).astype(jnp.bfloat16)
    arrived_inputs, arrived_grads = dispatch(
        send_inputs.reshape(rows), send_grads.reshape(rows), parts
    )
    arrived_inputs, arrived_grads, mixer_output = lax.optimization_barrier(
        (arrived_inputs, arrived_grads, mixer_output)
    )
    all_mixer = lax.all_gather(mixer_output, "sp", axis=0, tiled=True)
    input_part, grad_gate, grad_up, grad_down = expert_terms(
        arrived_inputs.reshape(peers * capacity, model_width),
        arrived_grads.reshape(peers * capacity, model_width),
        gate_weight[0],
        up_weight[0],
        down_weight[0],
    )
    place_blocks = places.reshape(peers, 1, capacity)
    combine = functools.reduce(
        jnp.logical_or, [slots[:, j][None, :, None] == place_blocks for j in range(TOP_K)]
    ).astype(jnp.bfloat16)
    residual_grad = return_rows(
        input_part.astype(jnp.bfloat16).reshape(peers, capacity, model_width),
        combine,
        my_cotangent,
    )
    grad_mix = jnp.dot(residual_grad, out_weight, preferred_element_type=jnp.float32).astype(
        jnp.bfloat16
    )
    slices = jnp.transpose(residual_grad.reshape(tok_dev, peers, model_width // peers), (1, 0, 2))
    gathered = []

    def exchange(total, logs):
        heads, head_dim, _ = total.shape
        packed = total.astype(jnp.bfloat16).reshape(-1, 128)
        wide = jnp.broadcast_to(logs[:, None], (heads, 128))
        all_res, all_tot, all_log = final_exchange(slices, packed, wide, parts)
        gathered.append(all_res)
        return all_tot.reshape((peers,) + total.shape), all_log[:, :, 0]

    grad_queries, grad_keys, grad_values = retention_grads(
        queries, key_vectors, value_vectors, grad_mix, log_decay, block_states, exchange
    )
    all_res = gathered[0].reshape(peers * tok_dev, model_width // peers)
    grad_out = contract_rows(all_res, all_mixer)
    return (
        grad_gate[None],
        grad_up[None],
        grad_down[None],
        grad_out,
        grad_queries,
        grad_keys,
        grad_values,
    )


def solution(mesh):
    return jax.shard_map(
        shards,
        mesh=mesh,
        in_specs=(
            P("sp", None),
            P("sp", None),
            P("sp", None),
            P("sp", None),
            P("sp", None, "tp"),
            P("sp", None, "tp"),
            P("sp", "tp", None),
            P(None, "tp"),
            P("sp", "tp"),
            P("sp", "tp"),
            P("sp", "tp"),
            P("sp", "tp"),
            P("sp", "tp"),
            P("sp", "tp", None, None),
        ),
        out_specs=(
            P("sp", None, "tp"),
            P("sp", None, "tp"),
            P("sp", "tp", None),
            P("sp", "tp"),
            P("sp", "tp"),
            P("sp", "tp"),
            P("sp", "tp"),
        ),
        check_vma=False,
    )
```

```python
import functools

import jax
import jax.numpy as jnp
from jax import lax
from jax.experimental import pallas as pl
from jax.experimental.pallas import tpu as pltpu
from jax.sharding import PartitionSpec as P

TOP_K = 2
MESH = pl.DeviceIdType.MESH
VMEM = pl.BlockSpec(memory_space=pltpu.VMEM)
ANY = pl.BlockSpec(memory_space=pl.ANY)

clamp_limit = 7.0
sigmoid_sharpness = 1.702


def contract_rows(left, right):
    return lax.dot_general(
        left, right, (((0,), (0,)), ((), ())), preferred_element_type=jnp.float32
    )


def contract_cols(left, right):
    return lax.dot_general(
        left, right, (((1,), (1,)), ((), ())), preferred_element_type=jnp.float32
    )


def peer_order(peers):
    near = [k for k in range(1, peers) if k < peers // 2]
    far = [k for k in range(1, peers) if k >= peers // 2]
    order = []
    while near or far:
        if near:
            order.append(near.pop(0))
        if far:
            order.append(far.pop(0))
    return order


def greet(peers, sp, tp):
    barrier = pltpu.get_barrier_semaphore()
    others = [(sp ^ k, tp) for k in range(1, peers)] + [(sp, tp ^ 1), (sp, tp ^ 2)]
    for other in others:
        pl.semaphore_signal(barrier, inc=1, device_id=other, device_id_type=MESH)
    pl.semaphore_wait(barrier, len(others))


def remote(src, dst, sems, kind, at, device):
    return pltpu.make_async_remote_copy(
        src_ref=src,
        dst_ref=dst,
        send_sem=sems.at[(2 * kind,) + at],
        recv_sem=sems.at[(2 * kind + 1,) + at],
        device_id=device,
        device_id_type=MESH,
    )


def exchange_start(peers, sp, tp, arrays, source, chunk, sems, local_sems):
    order = peer_order(peers)
    owns, firsts = [], {}
    for k in order:
        for a, (src, dst) in enumerate(arrays):
            copy = remote(source(src, sp ^ k), chunk(dst, sp, tp), sems, 0, (a, k), (sp ^ k, tp))
            copy.start()
            firsts[a, k] = copy
    for a, (src, dst) in enumerate(arrays):
        copy = pltpu.make_async_copy(source(src, sp), chunk(dst, sp, tp), local_sems.at[a])
        copy.start()
        owns.append(copy)
    return order, owns, firsts


def exchange_finish(peers, sp, tp, arrays, source, chunk, sems, state):
    order, owns, firsts = state
    crossings, partners, forwards = {}, {}, {}

    def forward(k):
        for a, (_, dst) in enumerate(arrays):
            crossings[a, k].wait_recv()
            here = chunk(dst, sp ^ k, tp ^ 2)
            copy = remote(here, here, sems, 3, (a, k), (sp, tp ^ 1))
            copy.start()
            forwards[a, k] = copy

    steps = [0] + order
    for i, k in enumerate(steps):
        for a, (src, dst) in enumerate(arrays):
            there = chunk(dst, sp ^ k, tp)
            if k:
                firsts[a, k].wait_recv()
                here = there
            else:
                here = source(src, sp)
            copy = remote(here, there, sems, 1, (a, k), (sp, tp ^ 2))
            copy.start()
            crossings[a, k] = copy
            copy = remote(here, there, sems, 2, (a, k), (sp, tp ^ 1))
            copy.start()
            partners[a, k] = copy
        if i >= 1:
            forward(steps[i - 1])
    forward(steps[-1])
    for copy in owns:
        copy.wait()
    for group in (partners, forwards):
        for copy in group.values():
            copy.wait_recv()
    for group in (firsts, crossings, partners, forwards):
        for copy in group.values():
            copy.wait_send()


def dispatch_kernel(peers, x_ref, g_ref, ox_ref, og_ref, sems, local_sems):
    sp, tp = lax.axis_index("sp"), lax.axis_index("tp")
    width = x_ref.shape[2]
    greet(peers, sp, tp)

    def source(ref, s):
        return ref.at[s]

    def chunk(ref, s, t):
        return ref.at[s, :, pl.ds(pl.multiple_of(t * width, width), width)]

    arrays = ((x_ref, ox_ref), (g_ref, og_ref))
    state = exchange_start(peers, sp, tp, arrays, source, chunk, sems, local_sems)
    exchange_finish(peers, sp, tp, arrays, source, chunk, sems, state)


def dispatch(x, g, parts):
    peers, capacity, width = x.shape
    out = jax.ShapeDtypeStruct((peers, capacity, width * parts), jnp.bfloat16)
    return pl.pallas_call(
        functools.partial(dispatch_kernel, peers),
        out_shape=(out, out),
        in_specs=[ANY, ANY],
        out_specs=(ANY, ANY),
        scratch_shapes=[
            pltpu.SemaphoreType.DMA((8, 2, peers)),
            pltpu.SemaphoreType.DMA((2,)),
        ],
        compiler_params=pltpu.CompilerParams(collective_id=0, has_side_effects=True),
        name="dispatch",
    )(x, g)


def return_kernel(
    peers, part_ref, pick_ref, cot_ref, res_ref, rx1, acc, sb, rx2, fb, ret, sems, tail_sems
):
    sp, tp = lax.axis_index("sp"), lax.axis_index("tp")
    width = cot_ref.shape[1]
    greet(peers, sp, tp)
    steps = peer_order(peers)[::-1] + [0]

    def cols(t):
        return pl.ds(pl.multiple_of(t * width, width), width)

    firsts, crossings, homes = {}, {}, {}
    for k in steps:
        for half, t in ((0, tp ^ 1), (1, tp ^ 3)):
            copy = remote(
                part_ref.at[sp ^ k, :, cols(t)], rx1.at[half, k], sems, half, (k,), (sp, tp ^ 1)
            )
            copy.start()
            firsts[half, k] = copy

    def cross(k):
        firsts[1, k].wait_recv()
        sb[k] = (
            part_ref[sp ^ k, :, cols(tp ^ 2)].astype(jnp.float32)
            + rx1[1, k].astype(jnp.float32)
        ).astype(jnp.bfloat16)
        crossings[k] = remote(sb.at[k], rx2.at[k], sems, 2, (k,), (sp, tp ^ 2))
        crossings[k].start()
        firsts[0, k].wait_recv()
        acc[k] = part_ref[sp ^ k, :, cols(tp)].astype(jnp.float32) + rx1[0, k].astype(
            jnp.float32
        )

    def home(k):
        crossings[k].wait_recv()
        final = (acc[k] + rx2[k].astype(jnp.float32)).astype(jnp.bfloat16)
        if k:
            fb[k] = final
            homes[k] = remote(fb.at[k], ret.at[sp], sems, 3, (k,), (sp ^ k, tp))
            homes[k].start()
        else:
            ret[sp] = final

    for i, k in enumerate(steps):
        cross(k)
        if i >= 2:
            home(steps[i - 2])
    home(steps[-2])
    home(steps[-1])
    total = cot_ref[...].astype(jnp.float32)
    for k in [0] + [k for k in steps if k]:
        if k:
            homes[k].wait_recv()
        total = total + jnp.dot(
            pick_ref[sp ^ k], ret[sp ^ k], preferred_element_type=jnp.float32
        )
    res_ref[:, cols(tp)] = total.astype(jnp.bfloat16)
    mine = res_ref.at[:, cols(tp)]
    across = remote(mine, mine, tail_sems, 0, (), (sp, tp ^ 2))
    across.start()
    beside = remote(mine, mine, tail_sems, 1, (), (sp, tp ^ 1))
    beside.start()
    across.wait_recv()
    theirs = res_ref.at[:, cols(tp ^ 2)]
    onward = remote(theirs, theirs, tail_sems, 2, (), (sp, tp ^ 1))
    onward.start()
    beside.wait_recv()
    onward.wait_recv()
    for group in (firsts, crossings, homes):
        for copy in group.values():
            copy.wait_send()
    for copy in (across, beside, onward):
        copy.wait_send()


def return_rows(part, pick, cot):
    peers, capacity, full = part.shape
    tokens, width = cot.shape
    rows = (peers, capacity, width)
    return pl.pallas_call(
        functools.partial(return_kernel, peers),
        out_shape=jax.ShapeDtypeStruct((tokens, full), jnp.bfloat16),
        in_specs=[VMEM] * 3,
        out_specs=VMEM,
        scratch_shapes=[
            pltpu.VMEM((2,) + rows, jnp.bfloat16),
            pltpu.VMEM(rows, jnp.float32),
            pltpu.VMEM(rows, jnp.bfloat16),
            pltpu.VMEM(rows, jnp.bfloat16),
            pltpu.VMEM(rows, jnp.bfloat16),
            pltpu.VMEM(rows, jnp.bfloat16),
            pltpu.SemaphoreType.DMA((8, peers)),
            pltpu.SemaphoreType.DMA((6,)),
        ],
        compiler_params=pltpu.CompilerParams(
            collective_id=1, has_side_effects=True, vmem_limit_bytes=40 * 2**20
        ),
        name="return_rows",
    )(part, pick, cot)


def final_kernel(
    peers, parts, res_ref, tot_ref, log_ref, all_res, all_tot, all_log, sems, local_sems, st_sems
):
    sp, tp = lax.axis_index("sp"), lax.axis_index("tp")
    share = res_ref.shape[1] // parts
    greet(peers, sp, tp)

    def rows(t):
        return pl.ds(pl.multiple_of(t * share, share), share)

    def source(ref, s):
        return ref.at[s, rows(tp)]

    def chunk(ref, s, t):
        return ref.at[s, rows(t)]

    small = []
    for k in peer_order(peers):
        for i, (src, dst) in enumerate(((tot_ref, all_tot), (log_ref, all_log))):
            copy = remote(src, dst.at[sp], st_sems, i, (k,), (sp ^ k, tp))
            copy.start()
            small.append(copy)
    own = []
    for i, (src, dst) in enumerate(((tot_ref, all_tot), (log_ref, all_log))):
        copy = pltpu.make_async_copy(src, dst.at[sp], local_sems.at[1 + i])
        copy.start()
        own.append(copy)
    arrays = ((res_ref, all_res),)
    state = exchange_start(peers, sp, tp, arrays, source, chunk, sems, local_sems)
    exchange_finish(peers, sp, tp, arrays, source, chunk, sems, state)
    for copy in own + small:
        copy.wait()


def final_exchange(res, tot, logs, parts):
    peers = res.shape[0]
    return pl.pallas_call(
        functools.partial(final_kernel, peers, parts),
        out_shape=(
            jax.ShapeDtypeStruct(res.shape, res.dtype),
            jax.ShapeDtypeStruct((peers,) + tot.shape, tot.dtype),
            jax.ShapeDtypeStruct((peers,) + logs.shape, logs.dtype),
        ),
        in_specs=[ANY] * 3,
        out_specs=(ANY,) * 3,
        scratch_shapes=[
            pltpu.SemaphoreType.DMA((8, 1, peers)),
            pltpu.SemaphoreType.DMA((3,)),
            pltpu.SemaphoreType.DMA((4, peers)),
        ],
        compiler_params=pltpu.CompilerParams(collective_id=2, has_side_effects=True),
        name="final_exchange",
    )(res, tot, logs)


def pair_slots(routes, experts_total, capacity):
    flat_routes = routes.reshape(-1)
    onehot = (flat_routes[:, None] == jnp.arange(experts_total, dtype=jnp.int32)[None, :]).astype(
        jnp.int32
    )
    before = jnp.cumsum(onehot, axis=0) - onehot
    return flat_routes * capacity + jnp.sum(before * onehot, axis=1)


def expert_terms(expert_rows, expert_cotangent, w_gate, w_up, w_down):
    gate_pre = jnp.dot(expert_rows, w_gate, preferred_element_type=jnp.float32)
    up_pre = jnp.dot(expert_rows, w_up, preferred_element_type=jnp.float32)
    act_grad = contract_cols(expert_cotangent, w_down)
    clamped = jnp.minimum(gate_pre, clamp_limit)
    logistic = jax.nn.sigmoid(sigmoid_sharpness * clamped)
    linear = jnp.clip(up_pre, -clamp_limit, clamp_limit)
    activation = (clamped * logistic * (linear + 1.0)).astype(jnp.bfloat16)
    slope_term = logistic + sigmoid_sharpness * clamped * logistic * (1.0 - logistic)
    gate_grad = jnp.where(
        gate_pre < clamp_limit, act_grad * (linear + 1.0) * slope_term, 0.0
    ).astype(jnp.bfloat16)
    up_grad = jnp.where(jnp.abs(up_pre) < clamp_limit, act_grad * clamped * logistic, 0.0).astype(
        jnp.bfloat16
    )
    input_part = contract_cols(gate_grad, w_gate) + contract_cols(up_grad, w_up)
    return (
        input_part,
        contract_rows(expert_rows, gate_grad),
        contract_rows(expert_rows, up_grad),
        contract_rows(activation, expert_cotangent),
    )


def retention_grads(
    queries, key_vectors, value_vectors, grad_mix, log_decay, block_states, exchange
):
    tok_dev = queries.shape[0]
    heads_local = log_decay.shape[1]
    head_dim = queries.shape[1] // heads_local
    blocks = block_states.shape[0]
    block_rows = tok_dev // blocks
    block_shape = (blocks, block_rows, heads_local, head_dim)
    query_blocks = queries.reshape(block_shape)
    key_blocks = key_vectors.reshape(block_shape)
    value_blocks = value_vectors.reshape(block_shape)
    grad_blocks = grad_mix.reshape(block_shape)
    cumulative = jnp.cumsum(log_decay.reshape(blocks, block_rows, heads_local), axis=1)
    block_ends = cumulative[:, -1, :]
    to_end = jnp.exp(block_ends[:, None, :] - cumulative)
    from_start = jnp.exp(cumulative)
    per_attention_head = jnp.transpose(cumulative, (0, 2, 1))
    differences = per_attention_head[:, :, :, None] - per_attention_head[:, :, None, :]
    causal = (
        jnp.arange(block_rows, dtype=jnp.int32)[:, None]
        >= jnp.arange(block_rows, dtype=jnp.int32)[None, :]
    )
    decays = jnp.where(causal, jnp.exp(jnp.minimum(differences, 0.0)), 0.0)
    scaled_queries = (query_blocks * from_start[..., None]).astype(jnp.bfloat16)
    outer_terms = jnp.einsum(
        "nthd,nthe->nhde", scaled_queries, grad_blocks, preferred_element_type=jnp.float32
    )
    end_factor = jnp.exp(block_ends)
    ends_before = jnp.cumsum(block_ends, axis=0) - block_ends
    device_start = jnp.exp(cumulative + ends_before[:, None, :])
    total_queries = (query_blocks * device_start[..., None]).astype(jnp.bfloat16)
    local_total = jnp.einsum(
        "thd,the->hde",
        total_queries.reshape(tok_dev, heads_local, head_dim),
        grad_mix.reshape(tok_dev, heads_local, head_dim),
        preferred_element_type=jnp.float32,
    )
    all_totals, all_logs = exchange(local_total, jnp.sum(block_ends, axis=0))
    peers, place = lax.axis_size("sp"), lax.axis_index("sp")
    where = jnp.arange(peers, dtype=jnp.int32)
    between = ((where[None, :] > place) & (where[None, :] < where[:, None]))[..., None]
    reach = jnp.sum(jnp.where(between, all_logs[None], 0.0), axis=1)
    reach = jnp.where((where > place)[:, None], jnp.exp(reach), 0.0)
    suffix = jnp.sum(reach[:, :, None, None] * all_totals.astype(jnp.float32), axis=0)
    suffix = suffix.reshape(heads_local, head_dim, head_dim)
    grad_dot = jnp.einsum(
        "nthe,nshe->nhts", grad_blocks, value_blocks, preferred_element_type=jnp.float32
    )
    weighted_grad = (grad_dot * decays).astype(jnp.bfloat16)
    score_dot = jnp.einsum(
        "nthd,nshd->nhts", query_blocks, key_blocks, preferred_element_type=jnp.float32
    )
    weighted_score = (score_dot * decays).astype(jnp.bfloat16)
    query_intra = jnp.einsum(
        "nhts,nshd->nthd", weighted_grad, key_blocks, preferred_element_type=jnp.float32
    )
    query_carry = jnp.einsum(
        "nthe,nhde->nthd", grad_blocks, block_states, preferred_element_type=jnp.float32
    )
    grad_queries = (
        (query_intra + query_carry * from_start[..., None])
        .astype(jnp.bfloat16)
        .reshape(tok_dev, -1)
    )
    key_intra = jnp.einsum(
        "nhts,nthd->nshd", weighted_grad, query_blocks, preferred_element_type=jnp.float32
    )
    value_intra = jnp.einsum(
        "nhts,nthe->nshe", weighted_score, grad_blocks, preferred_element_type=jnp.float32
    )
    state_grad = suffix
    leaving = []
    for block_id in reversed(range(blocks)):
        leaving.append(state_grad)
        state_grad = end_factor[block_id][:, None, None] * state_grad + outer_terms[block_id]
    carried = jnp.stack(leaving[::-1], axis=0).astype(jnp.bfloat16)
    key_carry = jnp.einsum(
        "nshe,nhde->nshd", value_blocks, carried, preferred_element_type=jnp.float32
    )
    value_carry = jnp.einsum(
        "nshd,nhde->nshe", key_blocks, carried, preferred_element_type=jnp.float32
    )
    grad_keys = (
        (key_intra + key_carry * to_end[..., None]).astype(jnp.bfloat16).reshape(tok_dev, -1)
    )
    grad_values = (
        (value_intra + value_carry * to_end[..., None]).astype(jnp.bfloat16).reshape(tok_dev, -1)
    )
    return (grad_queries, grad_keys, grad_values)


def shards(
    moe_input,
    cotangent,
    routes,
    route_weights,
    gate_weight,
    up_weight,
    down_weight,
    out_weight,
    mixer_output,
    queries,
    key_vectors,
    value_vectors,
    log_decay,
    block_states,
):
    tok_dev, model_width = cotangent.shape
    peers, parts = lax.axis_size("sp"), lax.axis_size("tp")
    capacity = 5 * tok_dev * TOP_K // (4 * peers)
    slots = pair_slots(routes, peers, capacity).reshape(tok_dev, TOP_K)
    share_width = model_width // parts
    offset = lax.axis_index("tp") * share_width
    my_inputs = lax.dynamic_slice_in_dim(moe_input, offset, share_width, 1)
    my_cotangent = lax.dynamic_slice_in_dim(cotangent, offset, share_width, 1)
    places = jnp.arange(peers * capacity, dtype=jnp.int32)
    hits = [slots[:, j][None, :] == places[:, None] for j in range(TOP_K)]
    pick = functools.reduce(jnp.logical_or, hits).astype(jnp.bfloat16)
    slot_weight = sum(
        jnp.sum(jnp.where(hits[j], route_weights[:, j][None, :], 0.0), axis=1)
        for j in range(TOP_K)
    )
    rows = (peers, capacity, share_width)
    send_inputs = jnp.dot(pick, my_inputs, preferred_element_type=jnp.float32).astype(
        jnp.bfloat16
    )
    send_grads = (
        jnp.dot(pick, my_cotangent, preferred_element_type=jnp.float32) * slot_weight[:, None]
    ).astype(jnp.bfloat16)
    arrived_inputs, arrived_grads = dispatch(
        send_inputs.reshape(rows), send_grads.reshape(rows), parts
    )
    arrived_inputs, arrived_grads, mixer_output = lax.optimization_barrier(
        (arrived_inputs, arrived_grads, mixer_output)
    )
    all_mixer = lax.all_gather(mixer_output, "sp", axis=0, tiled=True)
    input_part, grad_gate, grad_up, grad_down = expert_terms(
        arrived_inputs.reshape(peers * capacity, model_width),
        arrived_grads.reshape(peers * capacity, model_width),
        gate_weight[0],
        up_weight[0],
        down_weight[0],
    )
    place_blocks = places.reshape(peers, 1, capacity)
    combine = functools.reduce(
        jnp.logical_or, [slots[:, j][None, :, None] == place_blocks for j in range(TOP_K)]
    ).astype(jnp.bfloat16)
    residual_grad = return_rows(
        input_part.astype(jnp.bfloat16).reshape(peers, capacity, model_width),
        combine,
        my_cotangent,
    )
    grad_mix = jnp.dot(residual_grad, out_weight, preferred_element_type=jnp.float32).astype(
        jnp.bfloat16
    )
    slices = jnp.transpose(residual_grad.reshape(tok_dev, peers, model_width // peers), (1, 0, 2))
    gathered = []

    def exchange(total, logs):
        heads, head_dim, _ = total.shape
        packed = total.astype(jnp.bfloat16).reshape(-1, 128)
        wide = jnp.broadcast_to(logs[:, None], (heads, 128))
        all_res, all_tot, all_log = final_exchange(slices, packed, wide, parts)
        gathered.append(all_res)
        return all_tot.reshape(peers, heads, -1, 128), all_log[:, :, 0]

    grad_queries, grad_keys, grad_values = retention_grads(
        queries, key_vectors, value_vectors, grad_mix, log_decay, block_states, exchange
    )
    all_res = gathered[0].reshape(peers * tok_dev, model_width // peers)
    grad_out = contract_rows(all_res, all_mixer)
    return (
        grad_gate[None],
        grad_up[None],
        grad_down[None],
        grad_out,
        grad_queries,
        grad_keys,
        grad_values,
    )


def solution(mesh):
    return jax.shard_map(
        shards,
        mesh=mesh,
        in_specs=(
            P("sp", None),
            P("sp", None),
            P("sp", None),
            P("sp", None),
            P("sp", None, "tp"),
            P("sp", None, "tp"),
            P("sp", "tp", None),
            P(None, "tp"),
            P("sp", "tp"),
            P("sp", "tp"),
            P("sp", "tp"),
            P("sp", "tp"),
            P("sp", "tp"),
            P("sp", "tp", None, None),
        ),
        out_specs=(
            P("sp", None, "tp"),
            P("sp", None, "tp"),
            P("sp", "tp", None),
            P("sp", "tp"),
            P("sp", "tp"),
            P("sp", "tp"),
            P("sp", "tp"),
        ),
        check_vma=False,
    )
```
